512 devices in a mesh: grp: 2 (over y), sp: 16 (over z), tp: 16 (over x, core).
Axes of the slice: x: 8, y: 2, z: 16, core: 2. Of those that a mesh axis runs over, the one named last changes fastest.
The devices are a block of a 8x16x16 slice.
Arguments:
- target: bfloat16 [4096, 2048], P(('grp', 'sp', 'tp')), parts along dimension 0, may hold values from -60 to 60
- source: bfloat16 [32768, 2048], P(('grp', 'sp', 'tp')), parts along dimension 0, may hold values from -120 to 120
- w_query: bfloat16 [2, 2048, 2048], P(None, None, 'tp'), may hold values from -0.176776695 to 0.176776695
- w_key: bfloat16 [2, 2048, 2048], P(None, None, 'tp'), may hold values from -0.176776695 to 0.176776695
- w_value: bfloat16 [2, 2048, 2048], P(None, None, 'tp'), may hold values from -0.125 to 0.125
- w_out: bfloat16 [2, 2048, 2048], P(None, 'tp'), may hold values from -0.125 to 0.125
- gains: float32 [2, 2, 2048], replicated, may hold values from 0.1 to 1.9
Outputs:
- mixed: bfloat16 [4096, 2048], P(('grp', 'sp', 'tp')), parts along dimension 0
The draws below stay inside these ranges and needn't reach their ends.
There are 2 independent parts, one for each index of `grp`. The reference program is written for one: setup_inputs(seed, part) draws one part's arguments, and reference() takes and returns one part's arrays. A program takes and returns all parts, laid end to end along the dimension named above; an argument that names none is the same for every part. Nothing has to cross between parts.
All inputs are finite; a program needn't handle non-finite values.
Results may differ from the reference program's by a relative error of at most 0.025.
Values may be sent and summed in bfloat16 or wider, within the bound.
No kernel may reach another device: no remote copies, remote signals or barrier semaphores. Data moves between devices by JAX's collectives and lax.ppermute only.
A program may use at most 128 MiB of HBM per device.

```python
import jax
import jax.numpy as jnp
from jax import lax

D = 2048
HEADS = 16
HEAD = 128
LAYERS = 2
TGT = 2048
SRC = 16384
N_TP = 16


def draw_target(key, part):
    base = jnp.clip(jax.random.normal(jax.random.fold_in(key, 11), (TGT, D), jnp.float32), -6.0, 6.0)
    return base.astype(jnp.bfloat16)


def draw_source(key, part):
    base = jnp.clip(jax.random.normal(jax.random.fold_in(key, 21), (SRC, D), jnp.float32), -6.0, 6.0)
    return base.astype(jnp.bfloat16)


def draw_w_query(key, part):
    shared = jnp.clip(jax.random.normal(jax.random.fold_in(key, 31), (LAYERS, D, D), jnp.float32), -6.0, 6.0)
    return (shared * D ** (-0.5)).astype(jnp.bfloat16)


def draw_w_key(key, part):
    fresh = jnp.clip(jax.random.normal(jax.random.fold_in(key, 32), (LAYERS, D, D), jnp.float32), -6.0, 6.0)
    return (fresh * D ** (-0.5)).astype(jnp.bfloat16)


def steps_of(key, extent, pieces, smallest, top_value):
    level = 1.0
    for dim, shards_of in pieces:
        steps = jax.random.uniform(jax.random.fold_in(jax.random.fold_in(key, 6), dim), (shards_of,), jnp.float32, smallest / len(pieces), top_value / len(pieces))
        level = level * jnp.repeat(jnp.exp(steps), extent[dim] // shards_of).reshape((-1,) + (1,) * (len(extent) - 1 - dim))
    return level


def bell_draw(rng, extent, width, bound, cuts=(), held_as=jnp.bfloat16):
    result = jax.random.normal(rng, extent, jnp.float32) * width
    if len(cuts) > 0:
        result = steps_of(rng, extent, cuts, -0.22, 0.18) * result
    return jnp.clip(result, min=-bound, max=bound).astype(held_as)


def setup_inputs(seed: int = 0, part: int = 0) -> dict:
    key_list = jax.random.split(jax.random.key(seed), 8)
    part_splits = jax.random.split(jax.random.fold_in(key_list[7], part), 8)
    return {
        "target": draw_target(jax.random.fold_in(jax.random.fold_in(key_list[7], part), 71), part),
        "source": draw_source(jax.random.fold_in(jax.random.fold_in(key_list[7], part), 71), part),
        "w_query": draw_w_query(jax.random.fold_in(key_list[7], 71), part),
        "w_key": draw_w_key(jax.random.fold_in(key_list[7], 71), part),
        "w_value": bell_draw(key_list[4], (LAYERS, D, D), D ** -0.5, 0.125, ((2, 16),)),
        "w_out": bell_draw(key_list[5], (LAYERS, D, D), D ** -0.5, 0.125, ((1, 16),)),
        "gains": jnp.clip(1.0 + 0.18 * jax.random.normal(key_list[6], (LAYERS, 2, D), jnp.float32), 0.1, 1.9),
    }


EPS = 1e-06

def normalize(row_block, gain_row):
    return row_block * lax.rsqrt(lax.optimization_barrier(jnp.mean(row_block * row_block, axis=-1, keepdims=True)) + EPS) * gain_row.astype(jnp.float32)

def attend_head(query_cols, key_cols, value_cols):
    scores = jnp.dot(query_cols, key_cols.T, preferred_element_type=jnp.float32) * HEAD ** (-0.5)
    row_peak = lax.optimization_barrier(jnp.max(scores, axis=1, keepdims=True))
    weights = jnp.exp(scores - row_peak)
    row_total = lax.optimization_barrier(jnp.sum(weights, axis=1, keepdims=True))
    summed = jnp.dot(weights.astype(jnp.bfloat16), value_cols, preferred_element_type=jnp.float32)
    return (summed / row_total).astype(jnp.bfloat16)

def reference(target, source, w_query, w_key, w_value, w_out, gains):
    stream = target.astype(jnp.float32)
    group_width = D // N_TP
    for layer_index in range(LAYERS):
        keys = jnp.dot(source, w_key[layer_index], preferred_element_type=jnp.float32).astype(jnp.bfloat16)
        values = jnp.dot(source, w_value[layer_index], preferred_element_type=jnp.float32).astype(jnp.bfloat16)
        normed = normalize(stream, gains[layer_index, 0]).astype(jnp.bfloat16)
        queries = jnp.dot(normed, w_query[layer_index], preferred_element_type=jnp.float32).astype(jnp.bfloat16)

        def one_head(head_index):
            offset = (head_index * HEAD).astype(jnp.int32)
            return attend_head(lax.dynamic_slice_in_dim(queries, offset, HEAD, 1), lax.dynamic_slice_in_dim(keys, offset, HEAD, 1), lax.dynamic_slice_in_dim(values, offset, HEAD, 1))
        heads_out = lax.map(one_head, jnp.arange(HEADS, dtype=jnp.int32))
        attended = jnp.transpose(heads_out, (1, 0, 2)).reshape(TGT, D)
        out_weight = w_out[layer_index]

        def add_group(running, group_index):
            offset = (group_index * group_width).astype(jnp.int32)
            partial_value = jnp.dot(lax.dynamic_slice_in_dim(attended, offset, group_width, 1), lax.dynamic_slice_in_dim(out_weight, offset, group_width, 0), preferred_element_type=jnp.float32)
            rounded = lax.optimization_barrier(partial_value.astype(jnp.bfloat16))
            return (running + rounded.astype(jnp.float32), None)
        projected, _ = lax.scan(add_group, jnp.zeros((TGT, D), jnp.float32), jnp.arange(N_TP, dtype=jnp.int32))
        stream = stream + normalize(projected, gains[layer_index, 1])
    return stream.astype(jnp.bfloat16)
```

```python
import functools

import jax
import jax.numpy as jnp
from jax import lax
from jax.experimental import pallas as pl
from jax.experimental.pallas import tpu as pltpu
from jax.sharding import Mesh
from jax.sharding import PartitionSpec as P

HEAD = 128
EPS = 1e-06
LOG2E = 1.4426950408889634
TP = ("x", "c")
ROWS = ("grp", "sp", "x", "c")
STATS = 8


def split3(v):
    hi = v.astype(jnp.bfloat16).astype(jnp.float32)
    mid = (v - hi).astype(jnp.bfloat16).astype(jnp.float32)
    return hi, mid, v - hi - mid


def attend_kernel(q_ref, k_ref, v_ref, o_ref):
    rows = q_ref.shape[1]
    scores = lax.dot_general(
        q_ref[0], k_ref[...], (((1,), (1,)), ((), ())), preferred_element_type=jnp.float32
    )
    scale = HEAD**-0.5 * LOG2E
    peak = jnp.max(scores, axis=1, keepdims=True)
    weights = jnp.exp2((scores - peak) * scale)
    total = jnp.sum(weights, axis=1, keepdims=True)
    summed = jnp.dot(weights.astype(jnp.bfloat16), v_ref[...], preferred_element_type=jnp.float32)
    o_ref[0, :rows, :] = (summed / total).astype(jnp.bfloat16)
    lane = lax.broadcasted_iota(jnp.int32, (rows, HEAD), 1)
    both = jnp.where(lane < STATS // 2, peak * scale, total)
    flat = jnp.transpose(both)[:STATS]
    hi, mid, low = split3(flat)
    row = lax.broadcasted_iota(jnp.int32, (STATS, rows), 0) % (STATS // 2)
    stats = jnp.where(row == 0, hi, jnp.where(row == 1, mid, low))
    o_ref[0, rows:, :] = stats.astype(jnp.bfloat16)


def attend(queries, projected, level, parts):
    blocks, rows, _ = queries.shape
    sources = projected.shape[0]
    return pl.pallas_call(
        attend_kernel,
        grid=(blocks,),
        in_specs=[
            pl.BlockSpec((1, rows, HEAD), lambda i: (i, 0, 0)),
            pl.BlockSpec((sources, HEAD), lambda i: (0, 2 * level)),
            pl.BlockSpec((sources, HEAD), lambda i: (0, 2 * level + 1)),
        ],
        out_specs=pl.BlockSpec((1, rows + STATS, HEAD), lambda i: (i, 0, 0)),
        out_shape=jax.ShapeDtypeStruct((blocks, rows + STATS, HEAD), jnp.bfloat16),
        cost_estimate=pl.CostEstimate(
            flops=4 * blocks * rows * sources * HEAD,
            bytes_accessed=4 * blocks * rows * HEAD + 4 * sources * HEAD,
            transcendentals=blocks * rows * sources,
        ),
        name="attend",
    )(queries, projected, projected)


def join_kernel(g_ref, o_ref):
    parts, rows = g_ref.shape[0], g_ref.shape[1] - STATS
    half = STATS // 2
    stats = g_ref[:, rows:, :].astype(jnp.float32)
    peaks = stats[:, 0] + stats[:, 1] + stats[:, 2]
    totals = stats[:, half] + stats[:, half + 1] + stats[:, half + 2]
    share = jnp.exp2(peaks - jnp.max(peaks, axis=0, keepdims=True)) * totals
    share = share / jnp.sum(share, axis=0, keepdims=True)
    columns = jnp.transpose(jnp.concatenate([share] * (rows // parts), axis=0))
    joined = jnp.zeros((rows, HEAD), jnp.float32)
    for part in range(parts):
        joined += columns[:, part : part + 1] * g_ref[part, :rows, :].astype(jnp.float32)
    o_ref[...] = joined.astype(jnp.bfloat16)


def join(gathered):
    parts, rows, _ = gathered.shape
    rows -= STATS
    return pl.pallas_call(
        join_kernel,
        out_shape=jax.ShapeDtypeStruct((rows, HEAD), jnp.bfloat16),
        cost_estimate=pl.CostEstimate(
            flops=2 * parts * rows * HEAD, bytes_accessed=2 * parts * rows * HEAD, transcendentals=0
        ),
        name="join",
    )(gathered)


def to_all(block, axis):
    copies = jnp.broadcast_to(block[None], (lax.axis_size(axis), *block.shape))
    return lax.all_to_all(copies, axis, 0, 0, tiled=True)


def normalize(row_block, gain_row):
    return (
        row_block
        * lax.rsqrt(jnp.mean(row_block * row_block, axis=-1, keepdims=True) + EPS)
        * gain_row
    )


def body(target, source, w_query, w_key, w_value, w_out, gains):
    depth, width, _ = w_query.shape
    own = target.shape[0]
    chips, cores = lax.axis_size("x"), lax.axis_size("c")
    block = own * chips * cores
    side = width // cores
    core = lax.axis_index("c")

    rows_here = lax.all_gather(source, TP, axis=0, tiled=True)
    w_sources = jnp.concatenate(
        [w for level in range(depth) for w in (w_key[level], w_value[level])], axis=1
    )
    projected_source = jnp.dot(rows_here, w_sources, preferred_element_type=jnp.float32).astype(
        jnp.bfloat16
    )
    w_mix = w_out.reshape(depth, HEAD, cores, side).transpose(2, 0, 1, 3)
    w_mix = lax.all_to_all(w_mix, "c", 0, 0, tiled=True)

    stream = target.astype(jnp.float32)
    for level in range(depth):
        normed = normalize(stream, gains[level, 0]).astype(jnp.bfloat16)
        normed = lax.all_gather(to_all(normed, "x"), "c").reshape(block, width)
        queries = jnp.dot(normed, w_query[level], preferred_element_type=jnp.float32)
        queries = to_all(queries.astype(jnp.bfloat16), "sp")
        partial = attend(queries, projected_source, level, lax.axis_size("sp"))
        attended = join(lax.all_to_all(partial, "sp", 0, 0, tiled=True))
        pair = lax.all_gather(attended, "c")
        mixed = sum(
            jnp.dot(pair[k], w_mix[k, level], preferred_element_type=jnp.float32)
            for k in range(cores)
        ).astype(jnp.bfloat16)
        mixed = mixed.reshape(cores, chips, own, side).transpose(1, 0, 2, 3)
        mixed = lax.all_to_all(mixed, "x", 0, 0, tiled=True)
        mixed = jnp.sum(mixed.astype(jnp.float32), axis=0)
        mixed = lax.all_gather(mixed, "c")
        mixed = lax.dynamic_index_in_dim(mixed, core, 1, keepdims=False)
        projected = mixed.transpose(1, 0, 2).reshape(own, width)
        stream = stream + normalize(projected, gains[level, 1])
    return stream.astype(jnp.bfloat16)


def solution(mesh):
    split = Mesh(
        mesh.devices.reshape(mesh.shape["grp"], mesh.shape["sp"], -1, 2), ROWS
    )
    placed = (
        P(ROWS, None),
        P(ROWS, None),
        P(None, None, TP),
        P(None, None, TP),
        P(None, None, TP),
        P(None, TP, None),
        P(),
    )
    return jax.shard_map(
        body, mesh=split, in_specs=placed, out_specs=P(ROWS, None), check_vma=False
    )
```

```python
import functools

import jax
import jax.numpy as jnp
from jax import lax
from jax.experimental import pallas as pl
from jax.experimental.pallas import tpu as pltpu
from jax.sharding import Mesh
from jax.sharding import PartitionSpec as P

HEAD = 128
EPS = 1e-06
LOG2E = 1.4426950408889634
TP = ("x", "c")
SP = ("far", "near")
ROWS = ("grp", "far", "near", "x", "c")
STATS = 8
BLOCK = 128
NEAR = 4


def split3(v):
    hi = v.astype(jnp.bfloat16).astype(jnp.float32)
    mid = (v - hi).astype(jnp.bfloat16).astype(jnp.float32)
    return hi, mid, v - hi - mid


def attend_kernel(rows, chunk, q_ref, k_ref, v_ref, o_ref, values_ref):
    sources = k_ref.shape[0]
    scale = HEAD**-0.5 * LOG2E
    half = STATS // 2
    values_ref[...] = jnp.transpose(v_ref[...].astype(jnp.float32)).astype(jnp.bfloat16)

    def step(index, carry):
        queries = q_ref[pl.ds(pl.multiple_of(index * rows, rows), rows), :]
        peak = total = out = None
        for at in range(0, sources, chunk):
            scores = lax.dot_general(
                k_ref[at : at + chunk, :],
                queries,
                (((1,), (1,)), ((), ())),
                preferred_element_type=jnp.float32,
            )
            top = jnp.max(scores, axis=0, keepdims=True)
            new = top if peak is None else jnp.maximum(peak, top)
            weights = jnp.exp2((scores - new) * scale)
            here = jnp.sum(weights, axis=0, keepdims=True)
            part = jnp.dot(
                values_ref[:, at : at + chunk],
                weights.astype(jnp.bfloat16),
                preferred_element_type=jnp.float32,
            )
            if peak is None:
                total, out = here, part
            else:
                fade = jnp.exp2((peak - new) * scale)
                total, out = total * fade + here, out * fade + part
            peak = new
        out = (out / total).astype(jnp.bfloat16)
        row = lax.broadcasted_iota(jnp.int32, (STATS, rows), 0)
        hi, mid, low = split3(jnp.where(row < half, peak * scale, total))
        stats = jnp.where(row % half == 0, hi, jnp.where(row % half == 1, mid, low))
        stats = stats.astype(jnp.bfloat16)
        first = index * (rows // BLOCK)
        for k in range(rows // BLOCK):
            lanes = slice(k * BLOCK, (k + 1) * BLOCK)
            o_ref[first + k, :HEAD, :] = out[:, lanes]
            o_ref[first + k, HEAD:, :] = stats[:, lanes]
        return carry

    lax.fori_loop(0, q_ref.shape[0] // rows, step, 0)


def attend(queries, projected):
    rows, sources = queries.shape[0], projected.shape[0]
    blocks = rows // BLOCK
    out = (blocks, HEAD + STATS, BLOCK)
    return pl.pallas_call(
        functools.partial(attend_kernel, min(rows, 512), min(sources, 1024)),
        grid=(1,),
        in_specs=[
            pl.BlockSpec((rows, HEAD), lambda i: (0, 0)),
            pl.BlockSpec((sources, HEAD), lambda i: (0, 0)),
            pl.BlockSpec((sources, HEAD), lambda i: (0, 1)),
        ],
        out_specs=pl.BlockSpec(out, lambda i: (0, 0, 0)),
        out_shape=jax.ShapeDtypeStruct(out, jnp.bfloat16),
        scratch_shapes=[pltpu.VMEM((HEAD, sources), jnp.bfloat16)],
        compiler_params=pltpu.CompilerParams(vmem_limit_bytes=32 * 2**20),
        cost_estimate=pl.CostEstimate(
            flops=4 * rows * sources * HEAD,
            bytes_accessed=4 * rows * HEAD + 4 * sources * HEAD,
            transcendentals=rows * sources,
        ),
        name="attend",
    )(queries, projected, projected)


def join_kernel(g_ref, o_ref):
    half = STATS // 2
    stats = g_ref[:, HEAD:, :].astype(jnp.float32)
    peaks = stats[:, 0] + stats[:, 1] + stats[:, 2]
    totals = stats[:, half] + stats[:, half + 1] + stats[:, half + 2]
    share = jnp.exp2(peaks - jnp.max(peaks, axis=0, keepdims=True)) * totals
    share = share / jnp.sum(share, axis=0, keepdims=True)
    joined = jnp.zeros((HEAD, BLOCK), jnp.float32)
    for part in range(g_ref.shape[0]):
        joined += share[part : part + 1] * g_ref[part, :HEAD, :].astype(jnp.float32)
    o_ref[...] = joined.astype(jnp.bfloat16)


def join(gathered):
    return pl.pallas_call(
        join_kernel,
        out_shape=jax.ShapeDtypeStruct((HEAD, BLOCK), jnp.bfloat16),
        cost_estimate=pl.CostEstimate(
            flops=2 * gathered.size, bytes_accessed=2 * gathered.size, transcendentals=0
        ),
        name="join",
    )(gathered)


def to_all(block, axis):
    copies = jnp.broadcast_to(block[None], (lax.axis_size(axis), *block.shape))
    return lax.all_to_all(copies, axis, 0, 0, tiled=True)


def normalize(row_block, gain_row):
    return (
        row_block
        * lax.rsqrt(jnp.mean(row_block * row_block, axis=-1, keepdims=True) + EPS)
        * gain_row
    )


def dot(a, b):
    return jnp.dot(a, b, preferred_element_type=jnp.float32)


def body(target, source, w_query, w_key, w_value, w_out, gains):
    depth, width, _ = w_query.shape
    own = target.shape[0]
    chips, cores = lax.axis_size("x"), lax.axis_size("c")
    block = own * chips * cores
    side = width // cores
    core = lax.axis_index("c")

    rows_here = lax.all_gather(source, TP, axis=0, tiled=True)
    projected_source = []
    for level in range(depth):
        both = jnp.concatenate([w_key[level], w_value[level]], axis=1)
        both = dot(rows_here, both).astype(jnp.bfloat16)
        if level > 0:
            both = lax.all_gather(both, "near", axis=0, tiled=True)
        projected_source.append(both)

    mine = lax.dynamic_slice_in_dim(w_out, core * side, side, 2)
    other = lax.dynamic_slice_in_dim(w_out, (1 - core) * side, side, 2)
    other = lax.ppermute(other, "c", [(0, 1), (1, 0)])
    w_mix = jnp.concatenate(
        [jnp.where(core == 0, mine, other), jnp.where(core == 0, other, mine)], axis=1
    )

    stream = target.astype(jnp.float32)
    for level in range(depth):
        normed = normalize(stream, gains[level, 0]).astype(jnp.bfloat16)
        normed = lax.all_gather(to_all(normed, "x"), "c").reshape(block, width)
        peers = SP if level == 0 else "far"
        queries = to_all(dot(normed, w_query[level]).astype(jnp.bfloat16), peers)
        if level == 0:
            queries, w_mix = lax.optimization_barrier((queries, w_mix))
        partial = attend(queries.reshape(-1, HEAD), projected_source[level])
        attended = join(lax.all_to_all(partial, peers, 0, 0, tiled=True))
        pair = lax.all_gather(attended, "c", axis=0, tiled=True)
        mixed = lax.dot_general(
            pair, w_mix[level], (((0,), (0,)), ((), ())), preferred_element_type=jnp.float32
        ).astype(jnp.bfloat16)
        mixed = mixed.reshape(cores, chips, own, side).transpose(1, 0, 2, 3)
        mixed = lax.all_to_all(mixed, "x", 0, 0, tiled=True)
        mixed = jnp.sum(mixed.astype(jnp.float32), axis=0)
        mixed = lax.all_gather(mixed, "c")
        mixed = lax.dynamic_index_in_dim(mixed, core, 1, keepdims=False)
        projected = mixed.transpose(1, 0, 2).reshape(own, width)
        stream = stream + normalize(projected, gains[level, 1])
    return stream.astype(jnp.bfloat16)


def solution(mesh):
    split = Mesh(
        mesh.devices.reshape(mesh.shape["grp"], mesh.shape["sp"] // NEAR, NEAR, -1, 2), ROWS
    )
    placed = (
        P(ROWS, None),
        P(ROWS, None),
        P(None, None, TP),
        P(None, None, TP),
        P(None, None, TP),
        P(None, TP, None),
        P(),
    )
    return jax.shard_map(
        body, mesh=split, in_specs=placed, out_specs=P(ROWS, None), check_vma=False
    )
```

```python
import functools

import jax
import jax.numpy as jnp
from jax import lax
from jax.experimental import pallas as pl
from jax.experimental.pallas import tpu as pltpu
from jax.sharding import Mesh
from jax.sharding import PartitionSpec as P

HEAD = 128
EPS = 1e-06
LOG2E = 1.4426950408889634
TP = ("x", "c")
SP = ("far", "mid", "near")
ROWS = ("grp", "far", "mid", "near", "x", "c")
STATS = 8
BLOCK = 128
PAIR = 2


def split3(v):
    hi = v.astype(jnp.bfloat16).astype(jnp.float32)
    mid = (v - hi).astype(jnp.bfloat16).astype(jnp.float32)
    return hi, mid, v - hi - mid


def attend_kernel(rows, chunk, q_ref, *refs):
    held = (len(refs) - 1) // 3
    k_refs, v_refs, o_ref, t_refs = refs[:held], refs[held : 2 * held], refs[2 * held], refs[2 * held + 1 :]
    sources = k_refs[0].shape[0]
    scale = HEAD**-0.5 * LOG2E
    half = STATS // 2
    for v_ref, t_ref in zip(v_refs, t_refs):
        t_ref[...] = jnp.transpose(v_ref[...].astype(jnp.float32)).astype(jnp.bfloat16)

    def step(index, carry):
        queries = q_ref[pl.ds(pl.multiple_of(index * rows, rows), rows), :]
        peak = total = out = None
        for k_ref, t_ref in zip(k_refs, t_refs):
            for at in range(0, sources, chunk):
                scores = lax.dot_general(
                    k_ref[at : at + chunk, :],
                    queries,
                    (((1,), (1,)), ((), ())),
                    preferred_element_type=jnp.float32,
                )
                top = jnp.max(scores, axis=0, keepdims=True)
                new = top if peak is None else jnp.maximum(peak, top)
                weights = jnp.exp2((scores - new) * scale)
                here = jnp.sum(weights, axis=0, keepdims=True)
                part = jnp.dot(
                    t_ref[:, at : at + chunk],
                    weights.astype(jnp.bfloat16),
                    preferred_element_type=jnp.float32,
                )
                if peak is None:
                    total, out = here, part
                else:
                    fade = jnp.exp2((peak - new) * scale)
                    total, out = total * fade + here, out * fade + part
                peak = new
        out = (out / total).astype(jnp.bfloat16)
        row = lax.broadcasted_iota(jnp.int32, (STATS, rows), 0)
        hi, mid, low = split3(jnp.where(row < half, peak * scale, total))
        stats = jnp.where(row % half == 0, hi, jnp.where(row % half == 1, mid, low))
        stats = stats.astype(jnp.bfloat16)
        first = index * (rows // BLOCK)
        for k in range(rows // BLOCK):
            lanes = slice(k * BLOCK, (k + 1) * BLOCK)
            o_ref[first + k, :HEAD, :] = out[:, lanes]
            o_ref[first + k, HEAD:, :] = stats[:, lanes]
        return carry

    lax.fori_loop(0, q_ref.shape[0] // rows, step, 0)


def attend(queries, *held):
    rows, sources = queries.shape[0], held[0].shape[0]
    blocks = rows // BLOCK
    out = (blocks, HEAD + STATS, BLOCK)
    return pl.pallas_call(
        functools.partial(attend_kernel, min(rows, 512), min(sources, 1024)),
        grid=(1,),
        in_specs=[
            pl.BlockSpec((rows, HEAD), lambda i: (0, 0)),
            *(pl.BlockSpec((sources, HEAD), lambda i: (0, 0)) for _ in held),
            *(pl.BlockSpec((sources, HEAD), lambda i: (0, 1)) for _ in held),
        ],
        out_specs=pl.BlockSpec(out, lambda i: (0, 0, 0)),
        out_shape=jax.ShapeDtypeStruct(out, jnp.bfloat16),
        scratch_shapes=[pltpu.VMEM((HEAD, sources), jnp.bfloat16) for _ in held],
        compiler_params=pltpu.CompilerParams(vmem_limit_bytes=32 * 2**20),
        cost_estimate=pl.CostEstimate(
            flops=4 * rows * sources * HEAD * len(held),
            bytes_accessed=4 * rows * HEAD + 4 * sources * HEAD * len(held),
            transcendentals=rows * sources * len(held),
        ),
        name="attend",
    )(queries, *held, *held)


def join_kernel(g_ref, o_ref):
    half = STATS // 2
    stats = g_ref[:, HEAD:, :].astype(jnp.float32)
    peaks = stats[:, 0] + stats[:, 1] + stats[:, 2]
    totals = stats[:, half] + stats[:, half + 1] + stats[:, half + 2]
    share = jnp.exp2(peaks - jnp.max(peaks, axis=0, keepdims=True)) * totals
    share = share / jnp.sum(share, axis=0, keepdims=True)
    joined = jnp.zeros((HEAD, BLOCK), jnp.float32)
    for part in range(g_ref.shape[0]):
        joined += share[part : part + 1] * g_ref[part, :HEAD, :].astype(jnp.float32)
    o_ref[...] = joined.astype(jnp.bfloat16)


def join(gathered):
    return pl.pallas_call(
        join_kernel,
        out_shape=jax.ShapeDtypeStruct((HEAD, BLOCK), jnp.bfloat16),
        cost_estimate=pl.CostEstimate(
            flops=2 * gathered.size, bytes_accessed=2 * gathered.size, transcendentals=0
        ),
        name="join",
    )(gathered)


def to_all(block, axis):
    copies = jnp.broadcast_to(block[None], (lax.axis_size(axis), *block.shape))
    return lax.all_to_all(copies, axis, 0, 0, tiled=True)


def normalize(row_block, gain_row):
    return (
        row_block
        * lax.rsqrt(jnp.mean(row_block * row_block, axis=-1, keepdims=True) + EPS)
        * gain_row
    )


def dot(a, b):
    return jnp.dot(a, b, preferred_element_type=jnp.float32)


def body(target, source, w_query, w_key, w_value, w_out, gains):
    depth, width, _ = w_query.shape
    own = target.shape[0]
    chips, cores = lax.axis_size("x"), lax.axis_size("c")
    block = own * chips * cores
    side = width // cores
    core = lax.axis_index("c")

    rows_here = lax.all_gather(source, TP, axis=0, tiled=True)

    def keys_values(level):
        both = jnp.concatenate([w_key[level], w_value[level]], axis=1)
        return dot(rows_here, both).astype(jnp.bfloat16)

    mine = lax.dynamic_slice_in_dim(w_out, core * side, side, 2)
    other = lax.dynamic_slice_in_dim(w_out, (1 - core) * side, side, 2)
    other = lax.ppermute(other, "c", [(0, 1), (1, 0)])
    w_mix = jnp.concatenate(
        [jnp.where(core == 0, mine, other), jnp.where(core == 0, other, mine)], axis=1
    )

    stream = target.astype(jnp.float32)
    for level in range(depth):
        normed = normalize(stream, gains[level, 0]).astype(jnp.bfloat16)
        normed = lax.all_gather(to_all(normed, "x"), "c").reshape(block, width)
        queries = dot(normed, w_query[level]).astype(jnp.bfloat16)
        if level == 0:
            here = keys_values(level)
            held = (here, lax.ppermute(here, "near", [(0, 1), (1, 0)]))
            peers = ("far", "mid")
            queries, w_mix = lax.optimization_barrier((to_all(queries, peers), w_mix))
        else:
            held = (lax.all_gather(keys_values(level), ("mid", "near"), axis=0, tiled=True),)
            peers = "far"
            queries = to_all(queries, peers)
        partial = attend(queries.reshape(-1, HEAD), *held)
        attended = join(lax.all_to_all(partial, peers, 0, 0, tiled=True))
        pair = lax.all_gather(attended, "c", axis=0, tiled=True)
        mixed = lax.dot_general(
            pair, w_mix[level], (((0,), (0,)), ((), ())), preferred_element_type=jnp.float32
        ).astype(jnp.bfloat16)
        mixed = mixed.reshape(cores, chips, own, side).transpose(1, 0, 2, 3)
        mixed = lax.all_to_all(mixed, "x", 0, 0, tiled=True)
        mixed = jnp.sum(mixed.astype(jnp.float32), axis=0)
        mixed = lax.all_gather(mixed, "c")
        mixed = lax.dynamic_index_in_dim(mixed, core, 1, keepdims=False)
        projected = mixed.transpose(1, 0, 2).reshape(own, width)
        stream = stream + normalize(projected, gains[level, 1])
    return stream.astype(jnp.bfloat16)


def solution(mesh):
    split = Mesh(
        mesh.devices.reshape(mesh.shape["grp"], -1, PAIR, PAIR, mesh.shape["tp"] // 2, 2), ROWS
    )
    placed = (
        P(ROWS, None),
        P(ROWS, None),
        P(None, None, TP),
        P(None, None, TP),
        P(None, None, TP),
        P(None, TP, None),
        P(),
    )
    return jax.shard_map(
        body, mesh=split, in_specs=placed, out_specs=P(ROWS, None), check_vma=False
    )
```

```python
import functools

import jax
import jax.numpy as jnp
from jax import lax
from jax.experimental import pallas as pl
from jax.experimental.pallas import tpu as pltpu
from jax.sharding import Mesh
from jax.sharding import PartitionSpec as P

HEAD = 128
EPS = 1e-06
LOG2E = 1.4426950408889634
TP = ("x", "c")
SP = ("far", "mid", "near")
ROWS = ("grp", "far", "mid", "near", "x", "c")
STATS = 8
BLOCK = 128
PAIR = 2
VMEM = pl.BlockSpec(memory_space=pltpu.VMEM)


def split3(v):
    hi = v.astype(jnp.bfloat16).astype(jnp.float32)
    mid = (v - hi).astype(jnp.bfloat16).astype(jnp.float32)
    return hi, mid, v - hi - mid


def attend_kernel(rows, chunk, q_ref, *refs):
    held = (len(refs) - 1) // 2
    k_refs, o_ref, t_refs = refs[:held], refs[held], refs[held + 1 :]
    sources = k_refs[0].shape[0]
    scale = HEAD**-0.5 * LOG2E
    half = STATS // 2
    for k_ref, t_ref in zip(k_refs, t_refs):
        t_ref[...] = jnp.transpose(k_ref[:, HEAD:].astype(jnp.float32)).astype(jnp.bfloat16)

    def step(index, carry):
        queries = q_ref[pl.ds(pl.multiple_of(index * rows, rows), rows), :]
        peak = total = out = None
        for k_ref, t_ref in zip(k_refs, t_refs):
            for at in range(0, sources, chunk):
                scores = lax.dot_general(
                    k_ref[at : at + chunk, :HEAD],
                    queries,
                    (((1,), (1,)), ((), ())),
                    preferred_element_type=jnp.float32,
                )
                top = jnp.max(scores, axis=0, keepdims=True)
                new = top if peak is None else jnp.maximum(peak, top)
                weights = jnp.exp2((scores - new) * scale)
                here = jnp.sum(weights, axis=0, keepdims=True)
                part = jnp.dot(
                    t_ref[:, at : at + chunk],
                    weights.astype(jnp.bfloat16),
                    preferred_element_type=jnp.float32,
                )
                if peak is None:
                    total, out = here, part
                else:
                    fade = jnp.exp2((peak - new) * scale)
                    total, out = total * fade + here, out * fade + part
                peak = new
        out = (out / total).astype(jnp.bfloat16)
        row = lax.broadcasted_iota(jnp.int32, (STATS, rows), 0)
        hi, mid, low = split3(jnp.where(row < half, peak * scale, total))
        stats = jnp.where(row % half == 0, hi, jnp.where(row % half == 1, mid, low))
        stats = stats.astype(jnp.bfloat16)
        first = index * (rows // BLOCK)
        for k in range(rows // BLOCK):
            lanes = slice(k * BLOCK, (k + 1) * BLOCK)
            o_ref[first + k, :HEAD, :] = out[:, lanes]
            o_ref[first + k, HEAD:, :] = stats[:, lanes]
        return carry

    lax.fori_loop(0, q_ref.shape[0] // rows, step, 0)


def attend(queries, *held):
    rows, sources = queries.shape[0], held[0].shape[0]
    blocks = rows // BLOCK
    out = (blocks, HEAD + STATS, BLOCK)
    return pl.pallas_call(
        functools.partial(attend_kernel, min(rows, 512), min(sources, 1024)),
        in_specs=[VMEM] * (1 + len(held)),
        out_specs=VMEM,
        out_shape=jax.ShapeDtypeStruct(out, jnp.bfloat16),
        scratch_shapes=[pltpu.VMEM((HEAD, sources), jnp.bfloat16) for _ in held],
        compiler_params=pltpu.CompilerParams(vmem_limit_bytes=32 * 2**20),
        cost_estimate=pl.CostEstimate(
            flops=4 * rows * sources * HEAD * len(held),
            bytes_accessed=4 * rows * HEAD + 4 * sources * HEAD * len(held),
            transcendentals=rows * sources * len(held),
        ),
        name="attend",
    )(queries, *held)


def join_kernel(g_ref, o_ref):
    half = STATS // 2
    stats = g_ref[:, HEAD:, :].astype(jnp.float32)
    peaks = stats[:, 0] + stats[:, 1] + stats[:, 2]
    totals = stats[:, half] + stats[:, half + 1] + stats[:, half + 2]
    share = jnp.exp2(peaks - jnp.max(peaks, axis=0, keepdims=True)) * totals
    share = share / jnp.sum(share, axis=0, keepdims=True)
    joined = jnp.zeros((HEAD, BLOCK), jnp.float32)
    for part in range(g_ref.shape[0]):
        joined += share[part : part + 1] * g_ref[part, :HEAD, :].astype(jnp.float32)
    joined = jnp.transpose(joined).astype(jnp.bfloat16)
    for copy in range(o_ref.shape[0]):
        o_ref[copy] = joined


def join(gathered, copies):
    return pl.pallas_call(
        join_kernel,
        in_specs=[VMEM],
        out_specs=VMEM,
        out_shape=jax.ShapeDtypeStruct((copies, BLOCK, HEAD), jnp.bfloat16),
        cost_estimate=pl.CostEstimate(
            flops=2 * gathered.size, bytes_accessed=2 * gathered.size, transcendentals=0
        ),
        name="join",
    )(gathered)


def scaled(row_block, gain_row):
    return (
        row_block
        * lax.rsqrt(jnp.mean(row_block * row_block, axis=-1, keepdims=True) + EPS)
        * gain_row
    )


def query_kernel(level, stream_ref, mixed_ref, gains_ref, w_ref, q_ref, out_ref):
    stream = stream_ref[...].astype(jnp.float32)
    if mixed_ref is not None:
        cores = mixed_ref.shape[0]
        projected = jnp.concatenate([mixed_ref[k] for k in range(cores)], axis=1)
        stream = stream + scaled(projected.astype(jnp.float32), gains_ref[level - 1, 1:2, :])
        out_ref[...] = stream
    normed = scaled(stream, gains_ref[level, 0:1, :]).astype(jnp.bfloat16)
    queries = jnp.dot(normed, w_ref[level], preferred_element_type=jnp.float32).astype(jnp.bfloat16)
    for copy in range(q_ref.shape[0]):
        q_ref[copy] = queries


def query(level, stream, mixed, gains, w_query, copies):
    q_shape = jax.ShapeDtypeStruct((copies, stream.shape[0], HEAD), jnp.bfloat16)
    cost = pl.CostEstimate(
        flops=2 * stream.size * HEAD, bytes_accessed=8 * stream.size, transcendentals=0
    )
    params = pltpu.CompilerParams(vmem_limit_bytes=32 * 2**20)
    if mixed is None:

        def first(stream_ref, gains_ref, w_ref, q_ref):
            query_kernel(level, stream_ref, None, gains_ref, w_ref, q_ref, None)

        queries = pl.pallas_call(
            first,
            in_specs=[VMEM] * 3,
            out_specs=VMEM,
            out_shape=q_shape,
            cost_estimate=cost,
            compiler_params=params,
            name="query",
        )(stream, gains, w_query)
        return queries, stream
    return pl.pallas_call(
        functools.partial(query_kernel, level),
        in_specs=[VMEM] * 4,
        out_specs=(VMEM, VMEM),
        out_shape=(q_shape, jax.ShapeDtypeStruct(stream.shape, jnp.float32)),
        cost_estimate=cost,
        compiler_params=params,
        name="query",
    )(stream, mixed, gains, w_query)


def mix_kernel(heads_ref, w_ref, o_ref):
    cores, chips, rows, _ = heads_ref.shape
    total = jnp.zeros((rows, w_ref.shape[2]), jnp.float32)
    for chip in range(chips):
        pair = jnp.concatenate([heads_ref[core, chip] for core in range(cores)], axis=1)
        total += jnp.dot(pair, w_ref[chip], preferred_element_type=jnp.float32)
    total = total.astype(jnp.bfloat16)
    if len(o_ref.shape) == 2:
        o_ref[...] = total
    else:
        own = o_ref.shape[2]
        for chip in range(o_ref.shape[0]):
            for core in range(cores):
                at = (core * o_ref.shape[0] + chip) * own
                o_ref[chip, core] = total[at : at + own]


def mix(heads, weights, out):
    return pl.pallas_call(
        mix_kernel,
        in_specs=[VMEM, VMEM],
        out_specs=VMEM,
        out_shape=jax.ShapeDtypeStruct(out, jnp.bfloat16),
        cost_estimate=pl.CostEstimate(
            flops=2 * heads.size * weights.shape[2], bytes_accessed=2 * weights.size, transcendentals=0
        ),
        compiler_params=pltpu.CompilerParams(vmem_limit_bytes=32 * 2**20),
        name="mix",
    )(heads, weights)


def shifted(block, by):
    count = lax.axis_size(SP)
    return lax.ppermute(block, SP, [(k, (k + by) % count) for k in range(count)])


def dot(a, b):
    return jnp.dot(a, b, preferred_element_type=jnp.float32)


def spread(copies, axis):
    return lax.all_to_all(copies, axis, 0, 0, tiled=True)


def body(target, source, w_query, w_key, w_value, w_out, gains):
    depth, width, _ = w_query.shape
    own = target.shape[0]
    chips, cores = lax.axis_size("x"), lax.axis_size("c")
    block = own * chips * cores
    side = width // cores
    core = lax.axis_index("c")

    rows_here = lax.all_gather(source, TP, axis=0, tiled=True)

    def keys_values(level):
        both = jnp.concatenate([w_key[level], w_value[level]], axis=1)
        return dot(rows_here, both).astype(jnp.bfloat16)

    mine = lax.dynamic_slice_in_dim(w_out, core * side, side, 2)
    other = lax.dynamic_slice_in_dim(w_out, (1 - core) * side, side, 2)
    other = lax.ppermute(other, "c", [(0, 1), (1, 0)])
    first, second = jnp.where(core == 0, mine, other), jnp.where(core == 0, other, mine)
    w_mix = [jnp.concatenate([first[k], second[k]], axis=0) for k in range(depth)]

    stream = spread(jnp.broadcast_to(target[None], (chips, *target.shape)), "x")
    stream = lax.all_gather(stream, "c").reshape(block, width)
    mixed = None
    for level in range(depth):
        last = level == depth - 1
        peers = ("far", "mid") if level == 0 else ("far",)
        queries, stream = query(level, stream, mixed, gains, w_query, lax.axis_size(peers))
        queries = spread(queries, peers)
        if level == 0:
            here = keys_values(level)
            held = (here, lax.ppermute(here, "near", [(0, 1), (1, 0)]))
        partial = attend(queries.reshape(-1, HEAD), *held)
        attended = join(spread(partial, peers), 1 if last else chips)
        if not last:
            here = keys_values(level + 1)
            attended, here = lax.optimization_barrier((attended, here))
            above = shifted(here, -1)
            held = (here, shifted(here, 1), above, shifted(above, -1))
            w_whole = lax.all_gather(w_mix[level], "x")
            heads = lax.all_gather(spread(attended, "x"), "c")
            mixed = lax.all_gather(mix(heads, w_whole, (block, side)), "c")
        else:
            heads = lax.all_gather(attended, "c")
            mixed = mix(heads, w_mix[level][None], (chips, cores, own, side))
            mixed = jnp.sum(spread(mixed, "x").astype(jnp.float32), axis=0)
            mixed = lax.all_gather(mixed, "c")
            mixed = lax.dynamic_index_in_dim(mixed, core, 1, keepdims=False)
            projected = mixed.transpose(1, 0, 2).reshape(own, width)
            at = (core * chips + lax.axis_index("x")) * own
            stream = lax.dynamic_slice_in_dim(stream, at, own, 0)
            stream = stream + scaled(projected, gains[level, 1])
    return stream.astype(jnp.bfloat16)


def solution(mesh):
    split = Mesh(
        mesh.devices.reshape(mesh.shape["grp"], -1, PAIR, PAIR, mesh.shape["tp"] // 2, 2), ROWS
    )
    placed = (
        P(ROWS, None),
        P(ROWS, None),
        P(None, None, TP),
        P(None, None, TP),
        P(None, None, TP),
        P(None, TP, None),
        P(),
    )
    return jax.shard_map(
        body, mesh=split, in_specs=placed, out_specs=P(ROWS, None), check_vma=False
    )
```

```python
import functools

import jax
import jax.numpy as jnp
from jax import lax
from jax.experimental import pallas as pl
from jax.experimental.pallas import tpu as pltpu
from jax.sharding import Mesh
from jax.sharding import PartitionSpec as P

HEAD = 128
EPS = 1e-06
LOG2E = 1.4426950408889634
TP = ("x", "c")
SP = ("far", "mid", "near")
ROWS = ("grp", "far", "mid", "near", "x", "c")
STATS = 8
BLOCK = 128
PAIR = 2
VMEM = pl.BlockSpec(memory_space=pltpu.VMEM)


def split3(v):
    hi = v.astype(jnp.bfloat16).astype(jnp.float32)
    mid = (v - hi).astype(jnp.bfloat16).astype(jnp.float32)
    return hi, mid, v - hi - mid


def project_kernel(rows_ref, w_ref, *o_refs):
    out = jnp.dot(rows_ref[...], w_ref[...], preferred_element_type=jnp.float32)
    out = out.astype(jnp.bfloat16)
    each = 4 // len(o_refs)
    for k, o_ref in enumerate(o_refs):

        @pl.when(pl.program_id(0) // each == k)
        def _(o_ref=o_ref):
            o_ref[...] = out


def project(rows, weights, pieces):
    sources, width = rows.shape
    columns = weights.shape[1]
    step, each = sources // 4, 4 // pieces

    def place(piece):
        return lambda i: (jnp.clip(i - piece * each, 0, each - 1), 0)

    out = jax.ShapeDtypeStruct((sources // pieces, columns), jnp.bfloat16)
    return pl.pallas_call(
        project_kernel,
        grid=(4,),
        in_specs=[
            pl.BlockSpec((step, width), lambda i: (i, 0)),
            pl.BlockSpec((width, columns), lambda i: (0, 0)),
        ],
        out_specs=tuple(pl.BlockSpec((step, columns), place(k)) for k in range(pieces)),
        out_shape=(out,) * pieces,
        compiler_params=pltpu.CompilerParams(vmem_limit_bytes=58 * 2**20),
        cost_estimate=pl.CostEstimate(
            flops=2 * sources * width * columns, bytes_accessed=2 * rows.size, transcendentals=0
        ),
        name="project",
    )(rows, weights)


def attend_kernel(count, carried, final, *refs):
    q_ref, k_refs = refs[0], refs[1 : 1 + count]
    refs = refs[1 + count :]
    if carried:
        out_in, stats_in, refs = refs[0], refs[1], refs[2:]
    if final:
        o_ref, t_refs = refs[0], refs[1:]
    else:
        out_to, stats_to, t_refs = refs[0], refs[1], refs[2:]
    rows = min(q_ref.shape[0], 512)
    scale = HEAD**-0.5 * LOG2E
    half = STATS // 2
    for k_ref, t_ref in zip(k_refs, t_refs):
        t_ref[...] = jnp.transpose(k_ref[:, HEAD:].astype(jnp.float32)).astype(jnp.bfloat16)

    def step(index, carry):
        queries = q_ref[pl.ds(pl.multiple_of(index * rows, rows), rows), :]
        peak = total = out = None
        if carried:
            peak, total, out = stats_in[index, 0:1], stats_in[index, half : half + 1], out_in[index]
        for k_ref, t_ref in zip(k_refs, t_refs):
            scores = lax.dot_general(
                k_ref[:, :HEAD],
                queries,
                (((1,), (1,)), ((), ())),
                preferred_element_type=jnp.float32,
            )
            top = jnp.max(scores, axis=0, keepdims=True)
            new = top if peak is None else jnp.maximum(peak, top)
            weights = jnp.exp2((scores - new) * scale)
            here = jnp.sum(weights, axis=0, keepdims=True)
            part = jnp.dot(
                t_ref[...], weights.astype(jnp.bfloat16), preferred_element_type=jnp.float32
            )
            if peak is None:
                total, out = here, part
            else:
                fade = jnp.exp2((peak - new) * scale)
                total, out = total * fade + here, out * fade + part
            peak = new
        row = lax.broadcasted_iota(jnp.int32, (STATS, rows), 0)
        if not final:
            out_to[index] = out
            stats_to[index] = jnp.where(row < half, peak, total)
            return carry
        out = (out / total).astype(jnp.bfloat16)
        hi, mid, low = split3(jnp.where(row < half, peak * scale, total))
        stats = jnp.where(row % half == 0, hi, jnp.where(row % half == 1, mid, low))
        stats = stats.astype(jnp.bfloat16)
        first = index * (rows // BLOCK)
        for k in range(rows // BLOCK):
            lanes = slice(k * BLOCK, (k + 1) * BLOCK)
            o_ref[first + k, :HEAD, :] = out[:, lanes]
            o_ref[first + k, HEAD:, :] = stats[:, lanes]
        return carry

    lax.fori_loop(0, q_ref.shape[0] // rows, step, 0)


def attend(queries, held, state=None, final=True):
    total = queries.shape[0]
    rows = min(total, 512)
    if final:
        out = jax.ShapeDtypeStruct((total // BLOCK, HEAD + STATS, BLOCK), jnp.bfloat16)
    else:
        out = (
            jax.ShapeDtypeStruct((total // rows, HEAD, rows), jnp.float32),
            jax.ShapeDtypeStruct((total // rows, STATS, rows), jnp.float32),
        )
    carried = () if state is None else state
    sources = sum(piece.shape[0] for piece in held)
    return pl.pallas_call(
        functools.partial(attend_kernel, len(held), state is not None, final),
        in_specs=[VMEM] * (1 + len(held) + len(carried)),
        out_specs=VMEM if final else (VMEM, VMEM),
        out_shape=out,
        scratch_shapes=[pltpu.VMEM((HEAD, piece.shape[0]), jnp.bfloat16) for piece in held],
        compiler_params=pltpu.CompilerParams(vmem_limit_bytes=32 * 2**20),
        cost_estimate=pl.CostEstimate(
            flops=4 * total * sources * HEAD,
            bytes_accessed=4 * total * HEAD + 4 * sources * HEAD,
            transcendentals=total * sources,
        ),
        name="attend",
    )(queries, *held, *carried)


def join_kernel(g_ref, o_ref):
    half = STATS // 2
    stats = g_ref[:, HEAD:, :].astype(jnp.float32)
    peaks = stats[:, 0] + stats[:, 1] + stats[:, 2]
    totals = stats[:, half] + stats[:, half + 1] + stats[:, half + 2]
    share = jnp.exp2(peaks - jnp.max(peaks, axis=0, keepdims=True)) * totals
    share = share / jnp.sum(share, axis=0, keepdims=True)
    joined = jnp.zeros((HEAD, BLOCK), jnp.float32)
    for part in range(g_ref.shape[0]):
        joined += share[part : part + 1] * g_ref[part, :HEAD, :].astype(jnp.float32)
    joined = jnp.transpose(joined).astype(jnp.bfloat16)
    for copy in range(o_ref.shape[0]):
        o_ref[copy] = joined


def join(gathered, copies):
    return pl.pallas_call(
        join_kernel,
        in_specs=[VMEM],
        out_specs=VMEM,
        out_shape=jax.ShapeDtypeStruct((copies, BLOCK, HEAD), jnp.bfloat16),
        compiler_params=pltpu.CompilerParams(vmem_limit_bytes=8 * 2**20),
        cost_estimate=pl.CostEstimate(
            flops=2 * gathered.size, bytes_accessed=2 * gathered.size, transcendentals=0
        ),
        name="join",
    )(gathered)


def scaled(row_block, gain_row):
    return (
        row_block
        * lax.rsqrt(jnp.mean(row_block * row_block, axis=-1, keepdims=True) + EPS)
        * gain_row
    )


def query_kernel(level, stream_ref, mixed_ref, gains_ref, w_ref, q_ref, out_ref):
    stream = stream_ref[...].astype(jnp.float32)
    if mixed_ref is not None:
        cores = mixed_ref.shape[0]
        projected = jnp.concatenate([mixed_ref[k] for k in range(cores)], axis=1)
        stream = stream + scaled(projected.astype(jnp.float32), gains_ref[level - 1, 1:2, :])
        out_ref[...] = stream
    normed = scaled(stream, gains_ref[level, 0:1, :]).astype(jnp.bfloat16)
    queries = jnp.dot(normed, w_ref[level], preferred_element_type=jnp.float32).astype(jnp.bfloat16)
    for copy in range(q_ref.shape[0]):
        q_ref[copy] = queries


def query(level, stream, mixed, gains, w_query, copies):
    q_shape = jax.ShapeDtypeStruct((copies, stream.shape[0], HEAD), jnp.bfloat16)
    cost = pl.CostEstimate(
        flops=2 * stream.size * HEAD, bytes_accessed=8 * stream.size, transcendentals=0
    )
    params = pltpu.CompilerParams(vmem_limit_bytes=32 * 2**20)
    if mixed is None:

        def first(stream_ref, gains_ref, w_ref, q_ref):
            query_kernel(level, stream_ref, None, gains_ref, w_ref, q_ref, None)

        queries = pl.pallas_call(
            first,
            in_specs=[VMEM] * 3,
            out_specs=VMEM,
            out_shape=q_shape,
            cost_estimate=cost,
            compiler_params=params,
            name="query",
        )(stream, gains, w_query)
        return queries, stream
    return pl.pallas_call(
        functools.partial(query_kernel, level),
        in_specs=[VMEM] * 4,
        out_specs=(VMEM, VMEM),
        out_shape=(q_shape, jax.ShapeDtypeStruct(stream.shape, jnp.float32)),
        cost_estimate=cost,
        compiler_params=params,
        name="query",
    )(stream, mixed, gains, w_query)


def mix_kernel(heads_ref, w_ref, o_ref):
    cores, chips, rows, _ = heads_ref.shape
    total = jnp.zeros((rows, w_ref.shape[2]), jnp.float32)
    for chip in range(chips):
        pair = jnp.concatenate([heads_ref[core, chip] for core in range(cores)], axis=1)
        total += jnp.dot(pair, w_ref[chip], preferred_element_type=jnp.float32)
    total = total.astype(jnp.bfloat16)
    if len(o_ref.shape) == 2:
        o_ref[...] = total
    else:
        own = o_ref.shape[2]
        for chip in range(o_ref.shape[0]):
            for core in range(cores):
                at = (core * o_ref.shape[0] + chip) * own
                o_ref[chip, core] = total[at : at + own]


def mix(heads, weights, out):
    return pl.pallas_call(
        mix_kernel,
        in_specs=[VMEM, VMEM],
        out_specs=VMEM,
        out_shape=jax.ShapeDtypeStruct(out, jnp.bfloat16),
        cost_estimate=pl.CostEstimate(
            flops=2 * heads.size * weights.shape[2], bytes_accessed=2 * weights.size, transcendentals=0
        ),
        compiler_params=pltpu.CompilerParams(vmem_limit_bytes=32 * 2**20),
        name="mix",
    )(heads, weights)


def shifted(block, by):
    count = lax.axis_size(SP)
    return lax.ppermute(block, SP, [(k, (k + by) % count) for k in range(count)])


def spread(copies, axis):
    return lax.all_to_all(copies, axis, 0, 0, tiled=True)


def body(target, source, w_query, w_key, w_value, w_out, gains):
    depth, width, _ = w_query.shape
    own = target.shape[0]
    chips, cores = lax.axis_size("x"), lax.axis_size("c")
    block = own * chips * cores
    side = width // cores
    core = lax.axis_index("c")

    rows_here = lax.all_gather(source, TP, axis=0, tiled=True)

    def keys_values(level, pieces):
        both = jnp.concatenate([w_key[level], w_value[level]], axis=1)
        return project(rows_here, both, pieces)

    mine = lax.dynamic_slice_in_dim(w_out, core * side, side, 2)
    other = lax.dynamic_slice_in_dim(w_out, (1 - core) * side, side, 2)
    other = lax.ppermute(other, "c", [(0, 1), (1, 0)])
    first, second = jnp.where(core == 0, mine, other), jnp.where(core == 0, other, mine)
    w_mix = [jnp.concatenate([first[k], second[k]], axis=0) for k in range(depth)]

    stream = spread(jnp.broadcast_to(target[None], (chips, *target.shape)), "x")
    stream = lax.all_gather(stream, "c").reshape(block, width)
    mixed = None
    for level in range(depth):
        last = level == depth - 1
        peers = ("far", "mid") if level == 0 else ("far",)
        queries, stream = query(level, stream, mixed, gains, w_query, lax.axis_size(peers))
        queries = spread(queries, peers)
        queries = queries.reshape(-1, HEAD)
        if level == 0:
            first, second = keys_values(level, 2)
            sides = (shifted(second, 1), shifted(first, -1))
            state = attend(queries, (first, second), final=False)
            partial = attend(queries, sides, state)
        else:
            partial = attend(queries, held)
        attended = join(spread(partial, peers), 1 if last else chips)
        if not last:
            (here,) = keys_values(level + 1, 1)
            middle = here.shape[0] // 2
            attended, here = lax.optimization_barrier((attended, here))
            held = (
                here,
                shifted(here, 1),
                shifted(here, -1),
                shifted(here[middle:], 2),
                shifted(here[:middle], -2),
            )
            w_whole = lax.all_gather(w_mix[level], "x")
            heads = lax.all_gather(spread(attended, "x"), "c")
            mixed = lax.all_gather(mix(heads, w_whole, (block, side)), "c")
            mixed, held = lax.optimization_barrier((mixed, held))
        else:
            heads = lax.all_gather(attended, "c")
            mixed = mix(heads, w_mix[level][None], (chips, cores, own, side))
            mixed = jnp.sum(spread(mixed, "x").astype(jnp.float32), axis=0)
            mixed = lax.all_gather(mixed, "c")
            mixed = lax.dynamic_index_in_dim(mixed, core, 1, keepdims=False)
            projected = mixed.transpose(1, 0, 2).reshape(own, width)
            at = (core * chips + lax.axis_index("x")) * own
            stream = lax.dynamic_slice_in_dim(stream, at, own, 0)
            stream = stream + scaled(projected, gains[level, 1])
    return stream.astype(jnp.bfloat16)


def solution(mesh):
    split = Mesh(
        mesh.devices.reshape(mesh.shape["grp"], -1, PAIR, PAIR, mesh.shape["tp"] // 2, 2), ROWS
    )
    placed = (
        P(ROWS, None),
        P(ROWS, None),
        P(None, None, TP),
        P(None, None, TP),
        P(None, None, TP),
        P(None, TP, None),
        P(),
    )
    return jax.shard_map(
        body, mesh=split, in_specs=placed, out_specs=P(ROWS, None), check_vma=False
    )
```
